32 devices in a mesh: grp: 2 (over y), sp: 4 (over z), tp: 4 (over x, core).
Axes of the slice: x: 2, y: 2, z: 4, core: 2. Of those that a mesh axis runs over, the one named last changes fastest.
Arguments:
- tokens: bfloat16 [8, 1024, 4096], P(('grp', 'tp'), 'sp'), parts along dimension 0, may hold values from -8 to 8, as said below
- offsets: int32 [8], P(('grp', 'tp')), parts along dimension 0, may hold values from 0 to 4095
- in_gain: float32 [4096], replicated, may hold values from 0.1 to 1.9
- w_latent: bfloat16 [4096, 1024], P('sp'), may hold values from -0.09375 to 0.09375
- w_rope_key: bfloat16 [4096, 32], replicated, may hold values from -0.09375 to 0.09375
- kv_gain: float32 [1024], replicated, may hold values from 0.1 to 1.9
- w_up_key: bfloat16 [1024, 2048], P(None, 'tp'), may hold values from -0.1875 to 0.1875
- w_up_value: bfloat16 [1024, 2048], P(None, 'tp'), may hold values from -0.1875 to 0.1875
- q_nope: bfloat16 [8, 2048], P(('grp', 'sp'), 'tp'), parts along dimension 0, may hold values from -300 to 300, as said below
- q_rope: bfloat16 [8, 1024], P(('grp', 'sp'), 'tp'), parts along dimension 0, may hold values from -16 to 16
Outputs:
- keys: bfloat16 [8, 1024, 2048], P(('grp', 'sp'), None, 'tp'), parts along dimension 0
- values: bfloat16 [8, 1024, 2048], P(('grp', 'sp'), None, 'tp'), parts along dimension 0
- rope_keys: bfloat16 [8, 32, 1024], P(('grp', 'sp')), parts along dimension 0
- read: bfloat16 [8, 2048], P(('grp', 'sp'), 'tp'), parts along dimension 0
The draws below stay inside these ranges and needn't reach their ends.
There are 2 independent parts, one for each index of `grp`. The reference program is written for one: setup_inputs(seed, part) draws one part's arguments, and reference() takes and returns one part's arrays. A program takes and returns all parts, laid end to end along the dimension named above; an argument that names none is the same for every part. Nothing has to cross between parts.
Inputs may be any that keep to these rules, and one draw needn't show every extreme that they name: `tokens`: entries of the layer's input. `q_nope`: entries of the first decoding token's queries.
All inputs are finite; a program needn't handle non-finite values.
Results may differ from the reference program's by a relative error of at most 0.02.
Values may be sent and summed in bfloat16 or wider, within the bound.
A program may use at most 128 MiB of HBM per device.

```python
import jax
import jax.numpy as jnp
from jax import lax

D = 4096
HEADS = 32
HEAD = 64
ROPE = 32
KV_RANK = 1024
SEQS = 4
LEN = 1024


def draw_tokens(key, part):
    first, second = jax.random.split(jax.random.fold_in(key, 29))
    noise = jax.random.normal(first, (SEQS, LEN, D), jnp.float32)
    base = jnp.clip(noise, -6.0, 6.0)
    return base.astype(jnp.bfloat16)


def draw_q_nope(key, part):
    first, second = jax.random.split(jax.random.fold_in(key, 17))
    base = jax.random.normal(first, (SEQS, HEADS, HEAD), jnp.float32) * 4.0
    base = jnp.clip(base, -16.0, 16.0)
    return base.reshape(SEQS, HEADS * HEAD).astype(jnp.bfloat16)


def plant(array, key, low, largest):
    place = [jax.random.randint(jax.random.fold_in(key, axis), (), 0, length) for axis, length in enumerate(array.shape)]
    widest = array.shape.index(max(array.shape))
    neighbour = place[:widest] + [(place[widest] + 1) % array.shape[widest]] + place[widest + 1:]
    return array.at[tuple(place)].set(low).at[tuple(neighbour)].set(largest)


def block_levels(stream_key, extent, pieces, low, top_value):
    loudness = 1.0
    for dim, parts in pieces:
        steps = jax.random.uniform(jax.random.fold_in(jax.random.fold_in(stream_key, 6), dim), (parts,), jnp.float32, low / len(pieces), top_value / len(pieces))
        loudness = loudness * jnp.repeat(jnp.exp(steps), extent[dim] // parts).reshape((-1,) + (1,) * (len(extent) - 1 - dim))
    return loudness


def normal_values(key, extent, deviation, reach, shards=(), kind=jnp.bfloat16):
    drawn = deviation * jax.random.normal(key, extent, jnp.float32)
    if shards:
        drawn = drawn * block_levels(key, extent, shards, -0.22, 0.18)
    return jnp.clip(drawn, -reach, reach).astype(kind)


def setup_inputs(seed: int = 0, part: int = 0) -> dict:
    key_list = jax.random.split(jax.random.key(seed), 11)
    own_keys = jax.random.split(jax.random.fold_in(key_list[10], part), 11)
    return {
        "tokens": draw_tokens(jax.random.fold_in(jax.random.fold_in(key_list[10], part), 71), part),
        "offsets": plant(jax.random.randint(own_keys[1], (SEQS,), 0, 4096), jax.random.fold_in(own_keys[1], 1), 0, 4095).astype(jnp.int32),
        "in_gain": jnp.clip(1.0 + 0.18 * jax.random.normal(key_list[2], (D,), jnp.float32), 0.1, 1.9),
        "w_latent": normal_values(key_list[3], (D, KV_RANK), D ** -0.5, 0.09375, ((0, 4),)),
        "w_rope_key": normal_values(key_list[4], (D, ROPE), D ** -0.5, 0.09375),
        "kv_gain": jnp.clip(1.0 + 0.18 * jax.random.normal(key_list[5], (KV_RANK,), jnp.float32), 0.1, 1.9),
        "w_up_key": normal_values(key_list[6], (KV_RANK, HEADS * HEAD), KV_RANK ** -0.5, 0.1875, ((1, 4),)),
        "w_up_value": normal_values(key_list[7], (KV_RANK, HEADS * HEAD), KV_RANK ** -0.5, 0.1875, ((1, 4),)),
        "q_nope": draw_q_nope(jax.random.fold_in(jax.random.fold_in(key_list[10], part), 71), part),
        "q_rope": normal_values(own_keys[9], (SEQS, HEADS * ROPE), 4.0, 16.0, ((0, 4), (1, 4))),
    }


EPS = 1e-06

def rms_scale(values, gain):
    wide = values.astype(jnp.float32)
    return wide * lax.rsqrt(lax.optimization_barrier(jnp.mean(wide * wide, axis=-1, keepdims=True)) + EPS) * gain.astype(jnp.float32)

def rotate(raw, position):
    inverse = 10000.0 ** (-jnp.arange(0, ROPE, 2).astype(jnp.float32) / ROPE)
    angle = position.astype(jnp.float32)[:, None] * inverse[None, :]
    cosine, sine = (jnp.cos(angle), jnp.sin(angle))
    half = ROPE // 2
    first, second = (raw[:, :half], raw[:, half:])
    return jnp.concatenate([first * cosine - second * sine, second * cosine + first * sine], axis=-1)

def reference(tokens, offsets, in_gain, w_latent, w_rope_key, kv_gain, w_up_key, w_up_value, q_nope, q_rope):

    def one_prompt(args):
        prompt, start = args
        normed = rms_scale(prompt, in_gain).astype(jnp.bfloat16)
        latent_raw = jnp.dot(normed, w_latent, preferred_element_type=jnp.float32)
        latent = rms_scale(latent_raw, kv_gain).astype(jnp.bfloat16)
        rope_raw = jnp.dot(normed, w_rope_key, preferred_element_type=jnp.float32)
        position = start + jnp.arange(LEN, dtype=jnp.int32)
        rotated = rotate(rope_raw, position).astype(jnp.bfloat16)
        keys = jnp.dot(latent, w_up_key, preferred_element_type=jnp.float32).astype(jnp.bfloat16)
        values = jnp.dot(latent, w_up_value, preferred_element_type=jnp.float32).astype(jnp.bfloat16)
        return (keys, values, rotated.T)
    keys, values, rope_keys = lax.map(one_prompt, (tokens, offsets))
    query = q_nope.astype(jnp.float32).reshape(SEQS, HEADS, HEAD)
    rotary_q = q_rope.astype(jnp.float32).reshape(SEQS, HEADS, ROPE)
    keys_wide = keys.astype(jnp.float32).reshape(SEQS, LEN, HEADS, HEAD)
    scores = jnp.einsum('shd,sjhd->shj', query, keys_wide)
    scores = scores + jnp.einsum('shr,srj->shj', rotary_q, rope_keys.astype(jnp.float32))
    scores = scores / jnp.sqrt(jnp.float32(HEAD + ROPE))
    weights = jax.nn.softmax(scores, axis=-1).astype(jnp.bfloat16)
    values_wide = values.astype(jnp.float32).reshape(SEQS, LEN, HEADS, HEAD)
    read = jnp.einsum('shj,sjhd->shd', weights.astype(jnp.float32), values_wide)
    read = read.astype(jnp.bfloat16).reshape(SEQS, HEADS * HEAD)
    return (keys, values, rope_keys, read)
```

```python
import functools

import jax
import jax.numpy as jnp
from jax import lax
from jax.experimental import pallas as pl
from jax.experimental.pallas import tpu as pltpu
from jax.sharding import PartitionSpec as P

HEAD = 64
ROPE = 32
LANES = 128
CORES = 2


EPS = 1e-06
MESH = pl.DeviceIdType.MESH


def gather_kernel(
    n_grp,
    n_sp,
    n_tp,
    groups,
    tok_hbm,
    w_hbm,
    w_rope,
    in_gain,
    cosine,
    sine,
    lat_out,
    rope_out,
    tok,
    w_own,
    normed,
    wbuf,
    acc,
    own,
    own_rope,
    transit,
    local_sem,
    z_send,
    z_recv,
    a_send,
    a_recv,
    b_send,
    b_recv,
    c_send,
    c_recv,
    l_send,
    t_send,
    t_recv,
    x_send,
    d_send,
    l_recv,
):
    n_x = n_tp // CORES
    prompts, rows = own.shape[1:3]
    depth, cols = w_own.shape
    width = cols // groups
    chunk = wbuf.shape[5]
    y, z, t = lax.axis_index("grp"), lax.axis_index("sp"), lax.axis_index("tp")
    x, core = t // CORES, t % CORES
    rank = (core * n_x + x) * n_grp + y
    half = n_x // 2

    def tp_of(x_to, core_to):
        return {"tp": x_to * CORES + core_to}

    x_peers = [lax.rem(x + k, n_x) for k in range(1, n_x)]
    y_peers = [lax.rem(y + k, n_grp) for k in range(1, n_grp)]
    z_peers = [lax.rem(z + k, n_sp) for k in range(1, n_sp)]

    fetch_tok = pltpu.make_async_copy(tok_hbm, tok, local_sem.at[0])
    fetch_w = pltpu.make_async_copy(w_hbm, w_own, local_sem.at[1])
    fetch_tok.start()
    fetch_w.start()

    barrier = pltpu.get_barrier_semaphore()
    targets = (
        [tp_of(p, core) for p in x_peers]
        + [{"grp": p} for p in y_peers]
        + [{"sp": p} for p in z_peers]
        + [tp_of(x, 1 - core)]
    )
    for target in targets:
        pl.semaphore_signal(barrier, inc=1, device_id=target, device_id_type=MESH)
    pl.semaphore_wait(barrier, len(targets))

    finish = []

    def remote(src, dst, send, recv, device):
        return pltpu.make_async_remote_copy(
            src_ref=src,
            dst_ref=dst,
            send_sem=send,
            recv_sem=recv,
            device_id=device,
            device_id_type=MESH,
        )

    def arrived(ref, recv):
        remote(ref, ref, recv, recv, tp_of(x, 1 - core)).wait_recv()

    units = [(g, d) for g in range(groups) for d in range(1, n_sp)]

    def stage_z(u):
        g, d = units[u]
        copy = remote(
            w_hbm.at[pl.ds(rank * chunk, chunk), pl.ds(g * width, width)],
            wbuf.at[g, d - 1, core, x, y],
            z_send.at[u],
            z_recv.at[u],
            {"sp": lax.rem(z + n_sp - d, n_sp)},
        )
        copy.start()
        finish.append(copy.wait_send)

    def x_first(g):
        return g % 2 == 1

    def spread(u, src, send, recv, along_x):
        peers = x_peers if along_x else y_peers
        for k, peer in enumerate(peers):
            copy = remote(
                src,
                src,
                send.at[u, k],
                recv.at[u, k],
                tp_of(peer, core) if along_x else {"grp": peer},
            )
            copy.start()
            finish.append(copy.wait_send)

    def block_a(u):
        g, d = units[u]
        return wbuf.at[g, d - 1, core, x, y]

    def block_b(u):
        g, d = units[u]
        if x_first(g):
            return wbuf.at[g, d - 1, core, :, y]
        return wbuf.at[g, d - 1, core, x]

    def stage_a(u):
        arrived(block_a(u), z_recv.at[u])
        spread(u, block_a(u), a_send, a_recv, x_first(units[u][0]))

    def stage_b(u):
        g, _ = units[u]
        for k in range(len(x_peers if x_first(g) else y_peers)):
            arrived(block_a(u), a_recv.at[u, k])
        spread(u, block_b(u), b_send, b_recv, not x_first(g))

    def stage_c(u):
        g, d = units[u]
        for k in range(len(y_peers if x_first(g) else x_peers)):
            arrived(block_b(u), b_recv.at[u, k])
        ref = wbuf.at[g, d - 1, core]
        copy = remote(ref, ref, c_send.at[u], c_recv.at[u], tp_of(x, 1 - core))
        copy.start()
        finish.append(copy.wait_send)

    def stage_dot(u):
        g, d = units[u]
        arrived(wbuf.at[g, d - 1, core], c_recv.at[u])
        weight = wbuf[g, d - 1].reshape(depth, width)
        acc[g] += jnp.dot(
            normed[lax.rem(z + d, n_sp)], weight, preferred_element_type=jnp.float32
        )

    def crossing(m):
        return m % 2 == 0 and m > 0 and m < groups and n_x % 2 == 0

    def slot(m, s):
        if m == 0:
            return rope_out.at[s]
        return lat_out.at[s, :, pl.ds((m - 1) * width, width)]

    def mine(m, i):
        return own_rope.at[i] if m == 0 else own.at[m - 1, i]

    swapped = lax.rem(x + half, n_x) * CORES + core

    def stage_l(m):
        for i in range(prompts):
            home = t * prompts + i
            if crossing(m):
                copy = remote(
                    mine(m, i), transit.at[m, i], l_send.at[m, i], t_recv.at[m, i], {"tp": swapped}
                )
            else:
                copy = remote(
                    mine(m, i), slot(m, z), l_send.at[m, i], l_recv.at[m, z], {"sp": home}
                )
            pl.when(home != z)(copy.start)
            finish.append(lambda home=home, copy=copy: pl.when(home != z)(copy.wait_send))

    def stage_t(m):
        for i in range(prompts):
            home = swapped * prompts + i
            copy = remote(
                transit.at[m, i], slot(m, z), t_send.at[m, i], l_recv.at[m, z], {"sp": home}
            )

            def pass_on(m=m, i=i, copy=copy):
                arrived(transit.at[m, i], t_recv.at[m, i])
                copy.start()

            pl.when(home != z)(pass_on)
            finish.append(lambda home=home, copy=copy: pl.when(home != z)(copy.wait_send))

    owner = z // prompts

    def entry(m, e):
        x_in, core_in = owner // CORES, owner % CORES
        if crossing(m) and e > 0:
            x_in = lax.rem(x_in + half, n_x)
        return x_in, core_in

    def partner_copy(m, e):
        s = lax.rem(z + e, n_sp)
        return remote(slot(m, s), slot(m, s), d_send.at[m, e], l_recv.at[m, s], tp_of(x, 1 - core))

    def stage_x(m, e):
        s = lax.rem(z + e, n_sp)
        x_in, core_in = entry(m, e)
        here = (x == x_in) & (core == core_in)
        copies = [
            remote(slot(m, s), slot(m, s), x_send.at[m, e, k], l_recv.at[m, s], tp_of(peer, core))
            for k, peer in enumerate(x_peers)
        ]

        def enter():
            if e > 0:
                arrived(slot(m, s), l_recv.at[m, s])
            for copy in copies:
                copy.start()
            partner_copy(m, e).start()

        pl.when(here)(enter)

        def drain():
            for copy in copies:
                copy.wait_send()
            partner_copy(m, e).wait_send()

        finish.append(lambda: pl.when(here)(drain))

    def stage_d(m, e):
        s = lax.rem(z + e, n_sp)
        x_in, core_in = entry(m, e)
        here = (x != x_in) & (core == core_in)

        def hand():
            arrived(slot(m, s), l_recv.at[m, s])
            partner_copy(m, e).start()

        pl.when(here)(hand)
        finish.append(lambda: pl.when(here)(partner_copy(m, e).wait_send))

    def stage_end(m, e):
        s = lax.rem(z + e, n_sp)
        _, core_in = entry(m, e)
        pl.when(core != core_in)(lambda: arrived(slot(m, s), l_recv.at[m, s]))

    def finalize(m, value):
        value = value.reshape(prompts, rows, value.shape[-1])
        for i in range(prompts):
            mine(m, i)[...] = value[i]

            def keep(i=i):
                slot(m, z)[...] = value[i]

            pl.when(t * prompts + i == z)(keep)

    for u in range(len(units)):
        stage_z(u)

    fetch_tok.wait()
    step_rows = 16

    def norm(r, carry):
        at = pl.ds(pl.multiple_of(r * step_rows, step_rows), step_rows)
        wide = tok[at, :].astype(jnp.float32)
        scale = lax.rsqrt(jnp.mean(wide * wide, axis=-1, keepdims=True) + EPS)
        out = (wide * scale * in_gain[...]).astype(jnp.bfloat16)
        for b in range(n_sp):
            normed[b, at, :] = out[:, b * depth : (b + 1) * depth]
        return carry

    lax.fori_loop(0, prompts * rows // step_rows, norm, 0)

    work = {}

    def at_step(step, fn, *args):
        work.setdefault(step, []).append((fn, args))

    def own_dot(g):
        acc[g] = jnp.dot(
            normed[z], w_own[:, g * width : (g + 1) * width], preferred_element_type=jnp.float32
        )

    def rope_item():
        raw = jnp.dot(normed[0], w_rope[:depth, :], preferred_element_type=jnp.float32)
        for b in range(1, n_sp):
            raw += jnp.dot(
                normed[b], w_rope[b * depth : (b + 1) * depth, :], preferred_element_type=jnp.float32
            )
        other = pltpu.roll(raw, LANES - ROPE, 1)
        finalize(0, (raw * cosine[...] + other * sine[...]).astype(jnp.bfloat16))

    def group_item(g):
        finalize(g + 1, acc[g].astype(jnp.bfloat16))

    def route(m, step):
        at_step(step, stage_l, m)
        if crossing(m):
            at_step(step + 2, stage_t, m)
            step += 2
        for e in range(n_sp):
            at_step(step + 2, stage_x, m, e)
        for e in range(n_sp):
            at_step(step + 4, stage_d, m, e)

    lag_b, lag_c, lag_dot = 2, 4, 5
    for u, (g, d) in enumerate(units):
        at_step(u, stage_a, u)
        at_step(u + lag_b, stage_b, u)
        at_step(u + lag_c, stage_c, u)
    at_step(0, fetch_w.wait)
    for g in range(groups):
        at_step(g + 1, own_dot, g)
    at_step(1, rope_item)
    for u, (g, d) in enumerate(units):
        at_step(max(u + lag_dot, g + 1), stage_dot, u)
        if d == n_sp - 1:
            at_step(max(u + lag_dot, g + 1), group_item, g)
    route(0, 2)
    for g in range(groups):
        route(g + 1, max((g + 1) * (n_sp - 1) - 1 + lag_dot, g + 1))

    for step in sorted(work):
        for fn, args in work[step]:
            fn(*args)
    for m in range(groups + 1):
        for e in range(n_sp):
            stage_end(m, e)
    for fn in finish:
        fn()


def gather_latent(tokens, w_latent, w_rope, in_gain, cosine, sine):
    prompts, rows, width = tokens.shape
    n_grp, n_sp, n_tp = (lax.axis_size(a) for a in ("grp", "sp", "tp"))
    n_x = n_tp // CORES
    depth, cols = w_latent.shape
    groups = max(1, 16 // n_sp // 4 * 4) if n_sp <= 4 else 1
    part = cols // groups
    chunk = depth // (n_grp * n_tp)
    total = prompts * rows
    units = groups * (n_sp - 1)
    peers = max(n_x, n_grp) - 1
    items = groups + 1
    bf16, f32 = jnp.bfloat16, jnp.float32
    dma = pltpu.SemaphoreType.DMA
    vmem = pl.BlockSpec(memory_space=pltpu.VMEM)
    hbm = pl.BlockSpec(memory_space=pl.ANY)
    return pl.pallas_call(
        functools.partial(gather_kernel, n_grp, n_sp, n_tp, groups),
        out_shape=(
            jax.ShapeDtypeStruct((n_sp, rows, cols), bf16),
            jax.ShapeDtypeStruct((n_sp, rows, LANES), bf16),
        ),
        in_specs=[hbm, hbm, vmem, vmem, vmem, vmem],
        out_specs=(vmem, vmem),
        scratch_shapes=[
            pltpu.VMEM((total, width), bf16),
            pltpu.VMEM((depth, cols), bf16),
            pltpu.VMEM((n_sp, total, depth), bf16),
            pltpu.VMEM((groups, n_sp - 1, CORES, n_x, n_grp, chunk, part), bf16),
            pltpu.VMEM((groups, total, part), f32),
            pltpu.VMEM((groups, prompts, rows, part), bf16),
            pltpu.VMEM((prompts, rows, LANES), bf16),
            pltpu.VMEM((items, prompts, rows, part), bf16),
            dma((2,)),
            dma((units,)),
            dma((units,)),
            dma((units, peers)),
            dma((units, peers)),
            dma((units, peers)),
            dma((units, peers)),
            dma((units,)),
            dma((units,)),
            dma((items, prompts)),
            dma((items, prompts)),
            dma((items, prompts)),
            dma((items, n_sp, max(n_x - 1, 1))),
            dma((items, n_sp)),
            dma((items, n_sp)),
        ],
        compiler_params=pltpu.CompilerParams(
            collective_id=0, has_side_effects=True, vmem_limit_bytes=60 * 1024 * 1024
        ),
    )(tokens.reshape(total, width), w_latent, w_rope, in_gain, cosine, sine)


def cache_kernel(
    n_blocks,
    latent_ref,
    gain_ref,
    wk_ref,
    wv_ref,
    query_ref,
    rope_q_ref,
    rope_ref,
    keys_ref,
    values_ref,
    read_ref,
    scores,
    held,
):
    b = pl.program_id(0)
    rows = latent_ref.shape[1]
    raw = latent_ref[0].astype(jnp.float32)
    scale = lax.rsqrt(jnp.mean(raw * raw, axis=-1, keepdims=True) + EPS)
    latent = (raw * scale * gain_ref[...]).astype(jnp.bfloat16)
    keys = jnp.dot(latent, wk_ref[...], preferred_element_type=jnp.float32).astype(jnp.bfloat16)
    keys_ref[...] = keys
    values = jnp.dot(latent, wv_ref[...], preferred_element_type=jnp.float32).astype(jnp.bfloat16)
    values_ref[...] = values
    held[b] = values
    across = (((1,), (1,)), ((), ()))
    part = lax.dot_general(query_ref[...], keys, across, preferred_element_type=jnp.float32)
    part += lax.dot_general(
        rope_q_ref[...], rope_ref[0], across, preferred_element_type=jnp.float32
    )
    scores[b] = part / jnp.sqrt(jnp.float32(HEAD + ROPE))

    @pl.when(b == n_blocks - 1)
    def _():
        every = scores[...]
        peak = jnp.max(jnp.max(every, axis=-1, keepdims=True), axis=0, keepdims=True)
        expo = jnp.exp(every - peak)
        total = jnp.sum(jnp.sum(expo, axis=-1, keepdims=True), axis=0, keepdims=True)
        weights = (expo / total).astype(jnp.bfloat16)
        out = jnp.dot(weights[0], held[0], preferred_element_type=jnp.float32)
        for i in range(1, n_blocks):
            out += jnp.dot(weights[i], held[i], preferred_element_type=jnp.float32)
        head = lax.broadcasted_iota(jnp.int32, out.shape, 0)
        lane = lax.broadcasted_iota(jnp.int32, out.shape, 1)
        picked = jnp.where((lane >= head * HEAD) & (lane < head * HEAD + HEAD), out, 0.0)
        read_ref[...] = jnp.sum(picked, axis=0, keepdims=True).astype(jnp.bfloat16)


def fill_cache(latent, kv_gain, w_up_key, w_up_value, query, rotary_q, rope):
    n_blocks, rows, cols = latent.shape
    out_cols = w_up_key.shape[1]
    heads = query.shape[0]
    length = n_blocks * rows
    whole = lambda shape: pl.BlockSpec(shape, lambda b: (0,) * len(shape))
    return pl.pallas_call(
        functools.partial(cache_kernel, n_blocks),
        grid=(n_blocks,),
        out_shape=(
            jax.ShapeDtypeStruct((length, out_cols), jnp.bfloat16),
            jax.ShapeDtypeStruct((length, out_cols), jnp.bfloat16),
            jax.ShapeDtypeStruct((1, out_cols), jnp.bfloat16),
        ),
        in_specs=[
            pl.BlockSpec((1, rows, cols), lambda b: (b, 0, 0)),
            whole((1, cols)),
            whole((cols, out_cols)),
            whole((cols, out_cols)),
            whole(query.shape),
            whole(rotary_q.shape),
            pl.BlockSpec((1, rows, LANES), lambda b: (b, 0, 0)),
        ],
        out_specs=(
            pl.BlockSpec((rows, out_cols), lambda b: (b, 0)),
            pl.BlockSpec((rows, out_cols), lambda b: (b, 0)),
            whole((1, out_cols)),
        ),
        scratch_shapes=[
            pltpu.VMEM((n_blocks, heads, rows), jnp.float32),
            pltpu.VMEM((n_blocks, rows, out_cols), jnp.bfloat16),
        ],
    )(latent, kv_gain, w_up_key, w_up_value, query, rotary_q, rope)


def local(
    tokens, offsets, in_gain, w_latent, w_rope_key, kv_gain, w_up_key, w_up_value, q_nope, q_rope
):
    prompts, rows, _ = tokens.shape
    block = lax.axis_index("sp")
    half = ROPE // 2
    position = offsets[:, None] + block * rows + jnp.arange(rows, dtype=jnp.int32)[None, :]
    inverse = 10000.0 ** (-jnp.arange(0, ROPE, 2).astype(jnp.float32) / ROPE)
    angle = position.reshape(-1).astype(jnp.float32)[:, None] * inverse
    pad = ((0, 0), (0, LANES - ROPE))
    cosine, sine = jnp.cos(angle), jnp.sin(angle)
    cosine = jnp.pad(jnp.concatenate([cosine, cosine], axis=1), pad)
    sine = jnp.pad(jnp.concatenate([-sine, sine], axis=1), pad)
    w_rope = jnp.concatenate([w_rope_key, w_rope_key[:, half:], w_rope_key[:, :half]], axis=1)
    w_rope = jnp.pad(w_rope, ((0, 0), (0, LANES - 2 * ROPE)))
    latent, rope = gather_latent(tokens, w_latent, w_rope, in_gain[None], cosine, sine)

    heads = w_up_key.shape[1] // HEAD
    eye = jnp.eye(heads, dtype=q_nope.dtype)
    query = (eye[:, :, None] * q_nope.reshape(1, heads, HEAD)).reshape(heads, heads * HEAD)
    rotary_q = jnp.pad(q_rope.reshape(heads, ROPE), pad)
    keys, values, read = fill_cache(
        latent, kv_gain[None], w_up_key, w_up_value, query, rotary_q, rope
    )
    rope_keys = rope.reshape(-1, LANES)[:, :ROPE].T
    return (keys[None], values[None], rope_keys[None], read)


def solution(mesh):
    in_specs = (
        P(("grp", "tp"), "sp", None),
        P(("grp", "tp")),
        P(),
        P("sp", None),
        P(),
        P(),
        P(None, "tp"),
        P(None, "tp"),
        P(("grp", "sp"), "tp"),
        P(("grp", "sp"), "tp"),
    )
    out_specs = (
        P(("grp", "sp"), None, "tp"),
        P(("grp", "sp"), None, "tp"),
        P(("grp", "sp"), None, None),
        P(("grp", "sp"), "tp"),
    )
    return jax.shard_map(local, mesh=mesh, in_specs=in_specs, out_specs=out_specs, check_vma=False)
```

```python
import functools

import jax
import jax.numpy as jnp
import numpy as np
from jax import lax
from jax.experimental import pallas as pl
from jax.experimental.pallas import tpu as pltpu
from jax.sharding import PartitionSpec as P

HEAD = 64
ROPE = 32
LANES = 128
CORES = 2
GROUPS = 4
LAGS = (3, 6, 7)
HOP = 3


EPS = 1e-06
MESH = pl.DeviceIdType.MESH


def gather_kernel(
    n_grp,
    n_sp,
    n_tp,
    groups,
    tok_hbm,
    w_hbm,
    w_rope_hbm,
    in_gain,
    offsets,
    inverse,
    lat_out,
    rope_out,
    tok,
    w_own,
    w_rope,
    normed,
    wbuf,
    acc,
    own,
    own_rope,
    transit,
    local_sem,
    z_send,
    z_recv,
    a_send,
    a_recv,
    b_send,
    b_recv,
    c_send,
    c_recv,
    l_send,
    t_send,
    t_recv,
    x_send,
    d_send,
    l_recv,
):
    n_x = n_tp // CORES
    prompts, rows = own.shape[1:3]
    depth, cols = w_own.shape
    width = cols // groups
    chunk = wbuf.shape[5]
    y, z, t = lax.axis_index("grp"), lax.axis_index("sp"), lax.axis_index("tp")
    x, core = t // CORES, t % CORES
    rank = (core * n_x + x) * n_grp + y
    half = n_x // 2

    def tp_of(x_to, core_to):
        return {"tp": x_to * CORES + core_to}

    x_peers = [lax.rem(x + k, n_x) for k in range(1, n_x)]
    y_peers = [lax.rem(y + k, n_grp) for k in range(1, n_grp)]
    z_peers = [lax.rem(z + k, n_sp) for k in range(1, n_sp)]

    fetch_tok = pltpu.make_async_copy(tok_hbm, tok, local_sem.at[0])
    fetch_w = pltpu.make_async_copy(w_hbm, w_own, local_sem.at[1])
    fetch_rope = pltpu.make_async_copy(w_rope_hbm, w_rope, local_sem.at[2])
    fetch_tok.start()
    fetch_w.start()
    fetch_rope.start()

    barrier = pltpu.get_barrier_semaphore()
    targets = (
        [tp_of(p, core) for p in x_peers]
        + [{"grp": p} for p in y_peers]
        + [{"sp": p} for p in z_peers]
        + [tp_of(x, 1 - core)]
    )
    for target in targets:
        pl.semaphore_signal(barrier, inc=1, device_id=target, device_id_type=MESH)
    pl.semaphore_wait(barrier, len(targets))

    finish = []

    def remote(src, dst, send, recv, device):
        return pltpu.make_async_remote_copy(
            src_ref=src,
            dst_ref=dst,
            send_sem=send,
            recv_sem=recv,
            device_id=device,
            device_id_type=MESH,
        )

    def arrived(ref, recv):
        remote(ref, ref, recv, recv, tp_of(x, 1 - core)).wait_recv()

    units = [(g, d) for g in range(groups) for d in range(1, n_sp)]

    def stage_z(u):
        g, d = units[u]
        copy = remote(
            w_hbm.at[pl.ds(rank * chunk, chunk), pl.ds(g * width, width)],
            wbuf.at[g, d - 1, core, x, y],
            z_send.at[u],
            z_recv.at[u],
            {"sp": lax.rem(z + n_sp - d, n_sp)},
        )
        copy.start()
        finish.append(copy.wait_send)

    def x_first(u):
        return u % 2 == 1

    def spread(u, src, send, recv, along_x):
        peers = x_peers if along_x else y_peers
        for k, peer in enumerate(peers):
            copy = remote(
                src,
                src,
                send.at[u, k],
                recv.at[u, k],
                tp_of(peer, core) if along_x else {"grp": peer},
            )
            copy.start()
            finish.append(copy.wait_send)

    def block_a(u):
        g, d = units[u]
        return wbuf.at[g, d - 1, core, x, y]

    def block_b(u):
        g, d = units[u]
        if x_first(u):
            return wbuf.at[g, d - 1, core, :, y]
        return wbuf.at[g, d - 1, core, x]

    def stage_a(u):
        arrived(block_a(u), z_recv.at[u])
        spread(u, block_a(u), a_send, a_recv, x_first(u))

    def stage_b(u):
        g, _ = units[u]
        for k in range(len(x_peers if x_first(u) else y_peers)):
            arrived(block_a(u), a_recv.at[u, k])
        spread(u, block_b(u), b_send, b_recv, not x_first(u))

    def stage_c(u):
        g, d = units[u]
        for k in range(len(y_peers if x_first(u) else x_peers)):
            arrived(block_b(u), b_recv.at[u, k])
        ref = wbuf.at[g, d - 1, core]
        copy = remote(ref, ref, c_send.at[u], c_recv.at[u], tp_of(x, 1 - core))
        copy.start()
        finish.append(copy.wait_send)

    def stage_dot(u):
        g, d = units[u]
        arrived(wbuf.at[g, d - 1, core], c_recv.at[u])
        weight = wbuf[g, d - 1].reshape(depth, width)
        acc[g] += jnp.dot(
            normed[lax.rem(z + d, n_sp)], weight, preferred_element_type=jnp.float32
        )

    def crossing(m):
        return m % 2 == 0 and m > 0 and m < groups and n_x % 2 == 0

    def slot(m, s):
        if m == 0:
            return rope_out.at[s]
        return lat_out.at[s, :, pl.ds((m - 1) * width, width)]

    def mine(m, i):
        return own_rope.at[i] if m == 0 else own.at[m - 1, i]

    swapped = lax.rem(x + half, n_x) * CORES + core

    def stage_l(m):
        for i in range(prompts):
            home = t * prompts + i
            if crossing(m):
                copy = remote(
                    mine(m, i), transit.at[m, i], l_send.at[m, i], t_recv.at[m, i], {"tp": swapped}
                )
            else:
                copy = remote(
                    mine(m, i), slot(m, z), l_send.at[m, i], l_recv.at[m, z], {"sp": home}
                )
            pl.when(home != z)(copy.start)
            finish.append(lambda home=home, copy=copy: pl.when(home != z)(copy.wait_send))

    def stage_t(m):
        for i in range(prompts):
            home = swapped * prompts + i
            copy = remote(
                transit.at[m, i], slot(m, z), t_send.at[m, i], l_recv.at[m, z], {"sp": home}
            )

            def pass_on(m=m, i=i, copy=copy):
                arrived(transit.at[m, i], t_recv.at[m, i])
                copy.start()

            pl.when(home != z)(pass_on)
            finish.append(lambda home=home, copy=copy: pl.when(home != z)(copy.wait_send))

    owner = z // prompts

    def entry(m, e):
        x_in, core_in = owner // CORES, owner % CORES
        if crossing(m) and e > 0:
            x_in = lax.rem(x_in + half, n_x)
        return x_in, core_in

    def partner_copy(m, e):
        s = lax.rem(z + e, n_sp)
        return remote(slot(m, s), slot(m, s), d_send.at[m, e], l_recv.at[m, s], tp_of(x, 1 - core))

    def stage_x(m, e):
        s = lax.rem(z + e, n_sp)
        x_in, core_in = entry(m, e)
        here = (x == x_in) & (core == core_in)
        copies = [
            remote(slot(m, s), slot(m, s), x_send.at[m, e, k], l_recv.at[m, s], tp_of(peer, core))
            for k, peer in enumerate(x_peers)
        ]

        def enter():
            if e > 0:
                arrived(slot(m, s), l_recv.at[m, s])
            for copy in copies:
                copy.start()
            partner_copy(m, e).start()

        pl.when(here)(enter)

        def drain():
            for copy in copies:
                copy.wait_send()
            partner_copy(m, e).wait_send()

        finish.append(lambda: pl.when(here)(drain))

    def stage_d(m, e):
        s = lax.rem(z + e, n_sp)
        x_in, core_in = entry(m, e)
        here = (x != x_in) & (core == core_in)

        def hand():
            arrived(slot(m, s), l_recv.at[m, s])
            partner_copy(m, e).start()

        pl.when(here)(hand)
        finish.append(lambda: pl.when(here)(partner_copy(m, e).wait_send))

    def stage_end(m, e):
        s = lax.rem(z + e, n_sp)
        _, core_in = entry(m, e)
        pl.when(core != core_in)(lambda: arrived(slot(m, s), l_recv.at[m, s]))

    def finalize(m, value):
        value = value.reshape(prompts, rows, value.shape[-1])
        for i in range(prompts):
            mine(m, i)[...] = value[i]

            def keep(i=i):
                slot(m, z)[...] = value[i]

            pl.when(t * prompts + i == z)(keep)

    for u in range(len(units)):
        stage_z(u)

    step_rows, pieces = 16, 4

    def norm(r, carry):
        at = pl.ds(pl.multiple_of(r * step_rows, step_rows), step_rows)
        wide = tok[at, :].astype(jnp.float32)
        scale = lax.rsqrt(jnp.mean(wide * wide, axis=-1, keepdims=True) + EPS)
        out = (wide * scale * in_gain[...]).astype(jnp.bfloat16)
        for b in range(n_sp):
            normed[b, at, :] = out[:, b * depth : (b + 1) * depth]
        return carry

    def norm_piece(k):
        turns = prompts * rows // step_rows // pieces
        lax.fori_loop(k * turns, (k + 1) * turns, norm, 0)

    work = {}

    def at_step(step, fn, *args):
        work.setdefault(step, []).append((fn, args))

    def own_dot(g):
        acc[g] = jnp.dot(
            normed[z], w_own[:, g * width : (g + 1) * width], preferred_element_type=jnp.float32
        )

    def rope_item():
        fetch_rope.wait()
        raw = jnp.zeros((prompts * rows, ROPE), jnp.float32)
        for b in range(n_sp):
            raw += lax.dot_general(
                normed[b],
                w_rope[:, b * depth : (b + 1) * depth],
                (((1,), (1,)), ((), ())),
                preferred_element_type=jnp.float32,
            )
        half_rope = ROPE // 2
        blank = jnp.zeros((prompts * rows, LANES - ROPE), jnp.float32)
        lane = lax.broadcasted_iota(jnp.int32, (rows, LANES), 1)
        index = lax.broadcasted_iota(jnp.int32, (rows, LANES), 0)
        plain = jnp.concatenate([raw, blank], axis=1)
        other = jnp.concatenate([raw[:, half_rope:], raw[:, :half_rope], blank], axis=1)
        turned = []
        for i in range(prompts):
            position = offsets[i] + z * rows + index
            angle = position.astype(jnp.float32) * inverse[...]
            sine = jnp.sin(angle)
            sine = jnp.where(lane < half_rope, -sine, sine)
            at = slice(i * rows, (i + 1) * rows)
            turned.append(plain[at] * jnp.cos(angle) + other[at] * sine)
        finalize(0, jnp.concatenate(turned, axis=0).astype(jnp.bfloat16))

    def group_item(g):
        finalize(g + 1, acc[g].astype(jnp.bfloat16))

    def route(m, step):
        at_step(step, stage_l, m)
        if crossing(m):
            step += HOP
            at_step(step, stage_t, m)
        for e in range(n_sp):
            at_step(step + HOP, stage_x, m, e)
        for e in range(n_sp):
            at_step(step + 2 * HOP, stage_d, m, e)

    lag_b, lag_c, lag_dot = LAGS
    for u, (g, d) in enumerate(units):
        at_step(u, stage_a, u)
        at_step(u + lag_b, stage_b, u)
        at_step(u + lag_c, stage_c, u)
    at_step(0, fetch_tok.wait)
    for k in range(pieces):
        at_step(k, norm_piece, k)
    at_step(pieces, fetch_w.wait)
    at_step(pieces, rope_item)
    route(0, pieces)
    for u, (g, d) in enumerate(units):
        step = max(u + lag_dot, pieces)
        if d == 1:
            at_step(step, own_dot, g)
        at_step(step, stage_dot, u)
        if d == n_sp - 1:
            at_step(step, group_item, g)
            route(g + 1, step)

    for step in sorted(work):
        for fn, args in work[step]:
            fn(*args)
    for m in range(groups + 1):
        for e in range(n_sp):
            stage_end(m, e)
    for fn in finish:
        fn()


def gather_latent(tokens, w_latent, w_rope, in_gain, offsets, inverse):
    prompts, rows, width = tokens.shape
    n_grp, n_sp, n_tp = (lax.axis_size(a) for a in ("grp", "sp", "tp"))
    n_x = n_tp // CORES
    depth, cols = w_latent.shape
    groups = max(1, GROUPS * 3 // (n_sp - 1) // 4 * 4)
    part = cols // groups
    chunk = depth // (n_grp * n_tp)
    total = prompts * rows
    units = groups * (n_sp - 1)
    peers = max(n_x, n_grp) - 1
    items = groups + 1
    bf16, f32 = jnp.bfloat16, jnp.float32
    dma = pltpu.SemaphoreType.DMA
    vmem = pl.BlockSpec(memory_space=pltpu.VMEM)
    hbm = pl.BlockSpec(memory_space=pl.ANY)
    return pl.pallas_call(
        functools.partial(gather_kernel, n_grp, n_sp, n_tp, groups),
        out_shape=(
            jax.ShapeDtypeStruct((n_sp, rows, cols), bf16),
            jax.ShapeDtypeStruct((n_sp, rows, LANES), bf16),
        ),
        in_specs=[hbm, hbm, hbm, vmem, pl.BlockSpec(memory_space=pltpu.SMEM), vmem],
        out_specs=(vmem, vmem),
        scratch_shapes=[
            pltpu.VMEM((total, width), bf16),
            pltpu.VMEM((depth, cols), bf16),
            pltpu.VMEM((ROPE, width), bf16),
            pltpu.VMEM((n_sp, total, depth), bf16),
            pltpu.VMEM((groups, n_sp - 1, CORES, n_x, n_grp, chunk, part), bf16),
            pltpu.VMEM((groups, total, part), f32),
            pltpu.VMEM((groups, prompts, rows, part), bf16),
            pltpu.VMEM((prompts, rows, LANES), bf16),
            pltpu.VMEM((items, prompts, rows, part), bf16),
            dma((3,)),
            dma((units,)),
            dma((units,)),
            dma((units, peers)),
            dma((units, peers)),
            dma((units, peers)),
            dma((units, peers)),
            dma((units,)),
            dma((units,)),
            dma((items, prompts)),
            dma((items, prompts)),
            dma((items, prompts)),
            dma((items, n_sp, max(n_x - 1, 1))),
            dma((items, n_sp)),
            dma((items, n_sp)),
        ],
        compiler_params=pltpu.CompilerParams(
            collective_id=0, has_side_effects=True, vmem_limit_bytes=60 * 1024 * 1024
        ),
    )(tokens.reshape(total, width), w_latent, w_rope, in_gain, offsets, inverse)


def cache_kernel(
    n_blocks,
    latent_ref,
    gain_ref,
    wk_ref,
    wv_ref,
    q_nope_ref,
    q_rope_ref,
    rope_ref,
    keys_ref,
    values_ref,
    rope_keys_ref,
    read_ref,
    scores,
    held,
):
    b = pl.program_id(0)
    heads = scores.shape[1]

    def per_head(row, size):
        wide = jnp.broadcast_to(row.astype(jnp.float32), (heads, heads * size))
        head = lax.broadcasted_iota(jnp.int32, wide.shape, 0)
        lane = lax.broadcasted_iota(jnp.int32, wide.shape, 1)
        return jnp.where((lane >= head * size) & (lane < head * size + size), wide, 0.0)

    query = per_head(q_nope_ref[...], HEAD).astype(jnp.bfloat16)
    spread = (heads * ROPE, LANES)
    fold = lax.broadcasted_iota(jnp.int32, spread, 0) % ROPE == lax.broadcasted_iota(
        jnp.int32, spread, 1
    )
    rotary_q = jnp.dot(
        per_head(q_rope_ref[...], ROPE).astype(jnp.bfloat16),
        jnp.where(fold, 1.0, 0.0).astype(jnp.bfloat16),
        preferred_element_type=jnp.float32,
    ).astype(jnp.bfloat16)
    raw = latent_ref[0].astype(jnp.float32)
    scale = lax.rsqrt(jnp.mean(raw * raw, axis=-1, keepdims=True) + EPS)
    latent = (raw * scale * gain_ref[...]).astype(jnp.bfloat16)
    keys = jnp.dot(latent, wk_ref[...], preferred_element_type=jnp.float32).astype(jnp.bfloat16)
    keys_ref[...] = keys
    values = jnp.dot(latent, wv_ref[...], preferred_element_type=jnp.float32).astype(jnp.bfloat16)
    values_ref[...] = values
    held[b] = values
    rope = rope_ref[0]
    rope_keys_ref[...] = rope.astype(jnp.float32).T[:ROPE].astype(jnp.bfloat16)
    across = (((1,), (1,)), ((), ()))
    part = lax.dot_general(query, keys, across, preferred_element_type=jnp.float32)
    part += lax.dot_general(rotary_q, rope, across, preferred_element_type=jnp.float32)
    scores[b] = part / jnp.sqrt(jnp.float32(HEAD + ROPE))

    @pl.when(b == n_blocks - 1)
    def _():
        every = scores[...]
        peak = jnp.max(jnp.max(every, axis=-1, keepdims=True), axis=0, keepdims=True)
        expo = jnp.exp(every - peak)
        total = jnp.sum(jnp.sum(expo, axis=-1, keepdims=True), axis=0, keepdims=True)
        weights = (expo / total).astype(jnp.bfloat16)
        out = jnp.dot(weights[0], held[0], preferred_element_type=jnp.float32)
        for i in range(1, n_blocks):
            out += jnp.dot(weights[i], held[i], preferred_element_type=jnp.float32)
        head = lax.broadcasted_iota(jnp.int32, out.shape, 0)
        lane = lax.broadcasted_iota(jnp.int32, out.shape, 1)
        picked = jnp.where((lane >= head * HEAD) & (lane < head * HEAD + HEAD), out, 0.0)
        read_ref[...] = jnp.sum(picked, axis=0, keepdims=True).astype(jnp.bfloat16)


def fill_cache(latent, kv_gain, w_up_key, w_up_value, q_nope, q_rope, rope):
    n_blocks, rows, cols = latent.shape
    out_cols = w_up_key.shape[1]
    heads = out_cols // HEAD
    length = n_blocks * rows
    whole = lambda shape: pl.BlockSpec(shape, lambda b: (0,) * len(shape))
    return pl.pallas_call(
        functools.partial(cache_kernel, n_blocks),
        grid=(n_blocks,),
        out_shape=(
            jax.ShapeDtypeStruct((length, out_cols), jnp.bfloat16),
            jax.ShapeDtypeStruct((length, out_cols), jnp.bfloat16),
            jax.ShapeDtypeStruct((ROPE, length), jnp.bfloat16),
            jax.ShapeDtypeStruct((1, out_cols), jnp.bfloat16),
        ),
        in_specs=[
            pl.BlockSpec((1, rows, cols), lambda b: (b, 0, 0)),
            whole((1, cols)),
            whole((cols, out_cols)),
            whole((cols, out_cols)),
            whole(q_nope.shape),
            whole(q_rope.shape),
            pl.BlockSpec((1, rows, LANES), lambda b: (b, 0, 0)),
        ],
        out_specs=(
            pl.BlockSpec((rows, out_cols), lambda b: (b, 0)),
            pl.BlockSpec((rows, out_cols), lambda b: (b, 0)),
            pl.BlockSpec((ROPE, rows), lambda b: (0, b)),
            whole((1, out_cols)),
        ),
        scratch_shapes=[
            pltpu.VMEM((n_blocks, heads, rows), jnp.float32),
            pltpu.VMEM((n_blocks, rows, out_cols), jnp.bfloat16),
        ],
    )(latent, kv_gain, w_up_key, w_up_value, q_nope, q_rope, rope)


def local(
    tokens, offsets, in_gain, w_latent, w_rope_key, kv_gain, w_up_key, w_up_value, q_nope, q_rope
):
    frequency = np.float32(10000.0) ** (-np.arange(0, ROPE, 2).astype(np.float32) / ROPE)
    inverse = np.zeros((1, LANES), np.float32)
    inverse[0, :ROPE] = np.concatenate([frequency, frequency])
    inverse = jnp.asarray(inverse)
    latent, rope = gather_latent(tokens, w_latent, w_rope_key.T, in_gain[None], offsets, inverse)
    keys, values, rope_keys, read = fill_cache(
        latent, kv_gain[None], w_up_key, w_up_value, q_nope, q_rope, rope
    )
    return (keys[None], values[None], rope_keys[None], read)


def solution(mesh):
    in_specs = (
        P(("grp", "tp"), "sp", None),
        P(("grp", "tp")),
        P(),
        P("sp", None),
        P(),
        P(),
        P(None, "tp"),
        P(None, "tp"),
        P(("grp", "sp"), "tp"),
        P(("grp", "sp"), "tp"),
    )
    out_specs = (
        P(("grp", "sp"), None, "tp"),
        P(("grp", "sp"), None, "tp"),
        P(("grp", "sp"), None, None),
        P(("grp", "sp"), "tp"),
    )
    return jax.shard_map(local, mesh=mesh, in_specs=in_specs, out_specs=out_specs, check_vma=False)
```

```python
import functools

import jax
import jax.numpy as jnp
import numpy as np
from jax import lax
from jax.experimental import pallas as pl
from jax.experimental.pallas import tpu as pltpu
from jax.sharding import PartitionSpec as P

HEAD = 64
ROPE = 32
LANES = 128
CORES = 2
GROUPS = 4
LAGS = (3, 6, 7)
HOP = 3


EPS = 1e-06
MESH = pl.DeviceIdType.MESH


def gather_kernel(
    n_grp,
    n_sp,
    n_tp,
    groups,
    tok_hbm,
    w_hbm,
    w_rope_hbm,
    in_gain,
    offsets,
    inverse,
    lat_out,
    rope_out,
    tok,
    w_own,
    w_rope,
    normed,
    wbuf,
    acc,
    own,
    own_rope,
    transit,
    local_sem,
    own_send,
    z_send,
    z_recv,
    a_send,
    a_recv,
    b_send,
    b_recv,
    c_send,
    c_recv,
    l_send,
    t_send,
    t_recv,
    x_send,
    d_send,
    l_recv,
):
    n_x = n_tp // CORES
    prompts, rows = own.shape[1:3]
    depth, cols = w_own.shape
    width = cols // groups
    chunk = wbuf.shape[5]
    y, z, t = lax.axis_index("grp"), lax.axis_index("sp"), lax.axis_index("tp")
    x, core = t // CORES, t % CORES
    rank = (core * n_x + x) * n_grp + y
    half = n_x // 2

    def tp_of(x_to, core_to):
        return {"tp": x_to * CORES + core_to}

    x_peers = [lax.rem(x + k, n_x) for k in range(1, n_x)]
    y_peers = [lax.rem(y + k, n_grp) for k in range(1, n_grp)]
    z_peers = [lax.rem(z + k, n_sp) for k in range(1, n_sp)]

    fetch_tok = pltpu.make_async_copy(tok_hbm, tok, local_sem.at[0])
    fetch_w = pltpu.make_async_copy(w_hbm, w_own, local_sem.at[1])
    fetch_rope = pltpu.make_async_copy(w_rope_hbm, w_rope, local_sem.at[2])
    fetch_tok.start()
    fetch_w.start()
    fetch_rope.start()

    barrier = pltpu.get_barrier_semaphore()
    targets = (
        [tp_of(p, core) for p in x_peers]
        + [{"grp": p} for p in y_peers]
        + [{"sp": p} for p in z_peers]
        + [tp_of(x, 1 - core)]
    )
    for target in targets:
        pl.semaphore_signal(barrier, inc=1, device_id=target, device_id_type=MESH)
    pl.semaphore_wait(barrier, len(targets))

    finish = []

    def remote(src, dst, send, recv, device):
        return pltpu.make_async_remote_copy(
            src_ref=src,
            dst_ref=dst,
            send_sem=send,
            recv_sem=recv,
            device_id=device,
            device_id_type=MESH,
        )

    def arrived(ref, recv):
        remote(ref, ref, recv, recv, tp_of(x, 1 - core)).wait_recv()

    units = [(g, d) for g in range(groups) for d in range(1, n_sp)]
    above = n_sp - 1 - z
    both = jnp.minimum(z, above)

    def shard(d):
        paired = d <= 2 * both
        hop = jnp.where(paired, (d + 1) // 2, d - both)
        up = jnp.where(paired, d % 2 == 1, above > z)
        return jnp.where(up, z + hop, z - hop), up

    shards = {d: shard(d) for d in range(1, n_sp)}

    def own_z(g):
        for side, ahead, exists in ((0, z + 1, z + 1 < n_sp), (1, z + n_sp - 1, z > 0)):
            copy = remote(
                w_hbm.at[pl.ds(rank * chunk, chunk), pl.ds(g * width, width)],
                wbuf.at[g, z, core, x, y],
                own_send.at[g, side],
                z_recv.at[g, z],
                {"sp": lax.rem(ahead, n_sp)},
            )
            pl.when(exists)(copy.start)
            finish.append(lambda exists=exists, copy=copy: pl.when(exists)(copy.wait_send))

    def pass_z(u):
        g, d = units[u]
        s, up = shards[d]
        exists = jnp.where(up, z > 0, z + 1 < n_sp)
        ahead = jnp.where(up, z + n_sp - 1, z + 1)
        copy = remote(
            block_a(u),
            block_a(u),
            z_send.at[u],
            z_recv.at[g, s],
            {"sp": lax.rem(ahead, n_sp)},
        )
        pl.when(exists)(copy.start)
        finish.append(lambda: pl.when(exists)(copy.wait_send))

    def x_first(u):
        return u % 3 > 0

    def spread(u, src, send, recv, along_x):
        peers = x_peers if along_x else y_peers
        for k, peer in enumerate(peers):
            copy = remote(
                src,
                src,
                send.at[u, k],
                recv.at[u, k],
                tp_of(peer, core) if along_x else {"grp": peer},
            )
            copy.start()
            finish.append(copy.wait_send)

    def block_a(u):
        g, d = units[u]
        return wbuf.at[g, shards[d][0], core, x, y]

    def block_b(u):
        g, d = units[u]
        if x_first(u):
            return wbuf.at[g, shards[d][0], core, :, y]
        return wbuf.at[g, shards[d][0], core, x]

    def stage_a(u):
        arrived(block_a(u), z_recv.at[units[u][0], shards[units[u][1]][0]])
        pass_z(u)
        spread(u, block_a(u), a_send, a_recv, x_first(u))

    def stage_b(u):
        g, _ = units[u]
        for k in range(len(x_peers if x_first(u) else y_peers)):
            arrived(block_a(u), a_recv.at[u, k])
        spread(u, block_b(u), b_send, b_recv, not x_first(u))

    def stage_c(u):
        g, d = units[u]
        for k in range(len(y_peers if x_first(u) else x_peers)):
            arrived(block_b(u), b_recv.at[u, k])
        ref = wbuf.at[g, shards[d][0], core]
        copy = remote(ref, ref, c_send.at[u], c_recv.at[u], tp_of(x, 1 - core))
        copy.start()
        finish.append(copy.wait_send)

    def stage_dot(u):
        g, d = units[u]
        arrived(wbuf.at[g, shards[d][0], core], c_recv.at[u])
        s, _ = shards[d]
        weight = wbuf[g, s].reshape(depth, width)
        acc[g] += jnp.dot(
            normed[s], weight, preferred_element_type=jnp.float32
        )

    def crossing(m):
        return m % 2 == 0 and m > 0 and m < groups and n_x % 2 == 0

    def slot(m, s):
        if m == 0:
            return rope_out.at[s]
        return lat_out.at[s, :, pl.ds((m - 1) * width, width)]

    def mine(m, i):
        return own_rope.at[i] if m == 0 else own.at[m - 1, i]

    swapped = lax.rem(x + half, n_x) * CORES + core

    def stage_l(m):
        for i in range(prompts):
            home = t * prompts + i
            if crossing(m):
                copy = remote(
                    mine(m, i), transit.at[m, i], l_send.at[m, i], t_recv.at[m, i], {"tp": swapped}
                )
            else:
                copy = remote(
                    mine(m, i), slot(m, z), l_send.at[m, i], l_recv.at[m, z], {"sp": home}
                )
            pl.when(home != z)(copy.start)
            finish.append(lambda home=home, copy=copy: pl.when(home != z)(copy.wait_send))

    def stage_t(m):
        for i in range(prompts):
            home = swapped * prompts + i
            copy = remote(
                transit.at[m, i], slot(m, z), t_send.at[m, i], l_recv.at[m, z], {"sp": home}
            )

            def pass_on(m=m, i=i, copy=copy):
                arrived(transit.at[m, i], t_recv.at[m, i])
                copy.start()

            pl.when(home != z)(pass_on)
            finish.append(lambda home=home, copy=copy: pl.when(home != z)(copy.wait_send))

    owner = z // prompts

    def entry(m, e):
        x_in, core_in = owner // CORES, owner % CORES
        if crossing(m) and e > 0:
            x_in = lax.rem(x_in + half, n_x)
        return x_in, core_in

    def partner_copy(m, e):
        s = lax.rem(z + e, n_sp)
        return remote(slot(m, s), slot(m, s), d_send.at[m, e], l_recv.at[m, s], tp_of(x, 1 - core))

    def stage_x(m, e):
        s = lax.rem(z + e, n_sp)
        x_in, core_in = entry(m, e)
        here = (x == x_in) & (core == core_in)
        copies = [
            remote(slot(m, s), slot(m, s), x_send.at[m, e, k], l_recv.at[m, s], tp_of(peer, core))
            for k, peer in enumerate(x_peers)
        ]

        def enter():
            if e > 0:
                arrived(slot(m, s), l_recv.at[m, s])
            for copy in copies:
                copy.start()
            partner_copy(m, e).start()

        pl.when(here)(enter)

        def drain():
            for copy in copies:
                copy.wait_send()
            partner_copy(m, e).wait_send()

        finish.append(lambda: pl.when(here)(drain))

    def stage_d(m, e):
        s = lax.rem(z + e, n_sp)
        x_in, core_in = entry(m, e)
        here = (x != x_in) & (core == core_in)

        def hand():
            arrived(slot(m, s), l_recv.at[m, s])
            partner_copy(m, e).start()

        pl.when(here)(hand)
        finish.append(lambda: pl.when(here)(partner_copy(m, e).wait_send))

    def stage_end(m, e):
        s = lax.rem(z + e, n_sp)
        _, core_in = entry(m, e)
        pl.when(core != core_in)(lambda: arrived(slot(m, s), l_recv.at[m, s]))

    def finalize(m, value):
        value = value.reshape(prompts, rows, value.shape[-1])
        for i in range(prompts):
            mine(m, i)[...] = value[i]

            def keep(i=i):
                slot(m, z)[...] = value[i]

            pl.when(t * prompts + i == z)(keep)

    for g in range(groups):
        own_z(g)

    step_rows, pieces = 16, 4

    def norm(r, carry):
        at = pl.ds(pl.multiple_of(r * step_rows, step_rows), step_rows)
        wide = tok[at, :].astype(jnp.float32)
        scale = lax.rsqrt(jnp.mean(wide * wide, axis=-1, keepdims=True) + EPS)
        out = (wide * scale * in_gain[...]).astype(jnp.bfloat16)
        for b in range(n_sp):
            normed[b, at, :] = out[:, b * depth : (b + 1) * depth]
        return carry

    def norm_piece(k):
        turns = prompts * rows // step_rows // pieces
        lax.fori_loop(k * turns, (k + 1) * turns, norm, 0)

    work = {}

    def at_step(step, fn, *args):
        work.setdefault(step, []).append((fn, args))

    def own_dot(g):
        acc[g] = jnp.dot(
            normed[z], w_own[:, g * width : (g + 1) * width], preferred_element_type=jnp.float32
        )

    def rope_item():
        fetch_rope.wait()
        raw = jnp.zeros((prompts * rows, ROPE), jnp.float32)
        for b in range(n_sp):
            raw += lax.dot_general(
                normed[b],
                w_rope[:, b * depth : (b + 1) * depth],
                (((1,), (1,)), ((), ())),
                preferred_element_type=jnp.float32,
            )
        half_rope = ROPE // 2
        blank = jnp.zeros((prompts * rows, LANES - ROPE), jnp.float32)
        lane = lax.broadcasted_iota(jnp.int32, (rows, LANES), 1)
        index = lax.broadcasted_iota(jnp.int32, (rows, LANES), 0)
        plain = jnp.concatenate([raw, blank], axis=1)
        other = jnp.concatenate([raw[:, half_rope:], raw[:, :half_rope], blank], axis=1)
        turned = []
        for i in range(prompts):
            position = offsets[i] + z * rows + index
            angle = position.astype(jnp.float32) * inverse[...]
            sine = jnp.sin(angle)
            sine = jnp.where(lane < half_rope, -sine, sine)
            at = slice(i * rows, (i + 1) * rows)
            turned.append(plain[at] * jnp.cos(angle) + other[at] * sine)
        finalize(0, jnp.concatenate(turned, axis=0).astype(jnp.bfloat16))

    def group_item(g):
        finalize(g + 1, acc[g].astype(jnp.bfloat16))

    def route(m, step):
        at_step(step, stage_l, m)
        if crossing(m):
            step += HOP
            at_step(step, stage_t, m)
        for e in range(n_sp):
            at_step(step + HOP, stage_x, m, e)
        for e in range(n_sp):
            at_step(step + 2 * HOP, stage_d, m, e)

    lag_b, lag_c, lag_dot = LAGS
    for u, (g, d) in enumerate(units):
        at_step(u, stage_a, u)
        at_step(u + lag_b, stage_b, u)
        at_step(u + lag_c, stage_c, u)
    at_step(0, fetch_tok.wait)
    for k in range(pieces):
        at_step(k, norm_piece, k)
    at_step(pieces, fetch_w.wait)
    at_step(pieces, rope_item)
    route(0, pieces)
    for u, (g, d) in enumerate(units):
        step = max(u + lag_dot, pieces)
        if d == 1:
            at_step(step, own_dot, g)
        at_step(step, stage_dot, u)
        if d == n_sp - 1:
            at_step(step, group_item, g)
            route(g + 1, step)

    for step in sorted(work):
        for fn, args in work[step]:
            fn(*args)
    for m in range(groups + 1):
        for e in range(n_sp):
            stage_end(m, e)
    for fn in finish:
        fn()


def gather_latent(tokens, w_latent, w_rope, in_gain, offsets, inverse):
    prompts, rows, width = tokens.shape
    n_grp, n_sp, n_tp = (lax.axis_size(a) for a in ("grp", "sp", "tp"))
    n_x = n_tp // CORES
    depth, cols = w_latent.shape
    groups = max(1, GROUPS * 3 // (n_sp - 1) // 4 * 4)
    part = cols // groups
    chunk = depth // (n_grp * n_tp)
    total = prompts * rows
    units = groups * (n_sp - 1)
    peers = max(n_x, n_grp) - 1
    items = groups + 1
    bf16, f32 = jnp.bfloat16, jnp.float32
    dma = pltpu.SemaphoreType.DMA
    vmem = pl.BlockSpec(memory_space=pltpu.VMEM)
    hbm = pl.BlockSpec(memory_space=pl.ANY)
    return pl.pallas_call(
        functools.partial(gather_kernel, n_grp, n_sp, n_tp, groups),
        out_shape=(
            jax.ShapeDtypeStruct((n_sp, rows, cols), bf16),
            jax.ShapeDtypeStruct((n_sp, rows, LANES), bf16),
        ),
        in_specs=[hbm, hbm, hbm, vmem, pl.BlockSpec(memory_space=pltpu.SMEM), vmem],
        out_specs=(vmem, vmem),
        scratch_shapes=[
            pltpu.VMEM((total, width), bf16),
            pltpu.VMEM((depth, cols), bf16),
            pltpu.VMEM((ROPE, width), bf16),
            pltpu.VMEM((n_sp, total, depth), bf16),
            pltpu.VMEM((groups, n_sp, CORES, n_x, n_grp, chunk, part), bf16),
            pltpu.VMEM((groups, total, part), f32),
            pltpu.VMEM((groups, prompts, rows, part), bf16),
            pltpu.VMEM((prompts, rows, LANES), bf16),
            pltpu.VMEM((items, prompts, rows, part), bf16),
            dma((3,)),
            dma((groups, 2)),
            dma((units,)),
            dma((groups, n_sp)),
            dma((units, peers)),
            dma((units, peers)),
            dma((units, peers)),
            dma((units, peers)),
            dma((units,)),
            dma((units,)),
            dma((items, prompts)),
            dma((items, prompts)),
            dma((items, prompts)),
            dma((items, n_sp, max(n_x - 1, 1))),
            dma((items, n_sp)),
            dma((items, n_sp)),
        ],
        compiler_params=pltpu.CompilerParams(
            collective_id=0, has_side_effects=True, vmem_limit_bytes=60 * 1024 * 1024
        ),
    )(tokens.reshape(total, width), w_latent, w_rope, in_gain, offsets, inverse)


def cache_kernel(
    n_blocks,
    latent_ref,
    gain_ref,
    wk_ref,
    wv_ref,
    q_nope_ref,
    q_rope_ref,
    rope_ref,
    keys_ref,
    values_ref,
    rope_keys_ref,
    read_ref,
    scores,
    held,
):
    b = pl.program_id(0)
    heads = scores.shape[1]

    def per_head(row, size):
        wide = jnp.broadcast_to(row.astype(jnp.float32), (heads, heads * size))
        head = lax.broadcasted_iota(jnp.int32, wide.shape, 0)
        lane = lax.broadcasted_iota(jnp.int32, wide.shape, 1)
        return jnp.where((lane >= head * size) & (lane < head * size + size), wide, 0.0)

    query = per_head(q_nope_ref[...], HEAD).astype(jnp.bfloat16)
    spread = (heads * ROPE, LANES)
    fold = lax.broadcasted_iota(jnp.int32, spread, 0) % ROPE == lax.broadcasted_iota(
        jnp.int32, spread, 1
    )
    rotary_q = jnp.dot(
        per_head(q_rope_ref[...], ROPE).astype(jnp.bfloat16),
        jnp.where(fold, 1.0, 0.0).astype(jnp.bfloat16),
        preferred_element_type=jnp.float32,
    ).astype(jnp.bfloat16)
    raw = latent_ref[0].astype(jnp.float32)
    scale = lax.rsqrt(jnp.mean(raw * raw, axis=-1, keepdims=True) + EPS)
    latent = (raw * scale * gain_ref[...]).astype(jnp.bfloat16)
    keys = jnp.dot(latent, wk_ref[...], preferred_element_type=jnp.float32).astype(jnp.bfloat16)
    keys_ref[...] = keys
    values = jnp.dot(latent, wv_ref[...], preferred_element_type=jnp.float32).astype(jnp.bfloat16)
    values_ref[...] = values
    held[b] = values
    rope = rope_ref[0]
    rope_keys_ref[...] = rope.astype(jnp.float32).T[:ROPE].astype(jnp.bfloat16)
    across = (((1,), (1,)), ((), ()))
    part = lax.dot_general(query, keys, across, preferred_element_type=jnp.float32)
    part += lax.dot_general(rotary_q, rope, across, preferred_element_type=jnp.float32)
    scores[b] = part / jnp.sqrt(jnp.float32(HEAD + ROPE))

    @pl.when(b == n_blocks - 1)
    def _():
        every = scores[...]
        peak = jnp.max(jnp.max(every, axis=-1, keepdims=True), axis=0, keepdims=True)
        expo = jnp.exp(every - peak)
        total = jnp.sum(jnp.sum(expo, axis=-1, keepdims=True), axis=0, keepdims=True)
        weights = (expo / total).astype(jnp.bfloat16)
        out = jnp.dot(weights[0], held[0], preferred_element_type=jnp.float32)
        for i in range(1, n_blocks):
            out += jnp.dot(weights[i], held[i], preferred_element_type=jnp.float32)
        head = lax.broadcasted_iota(jnp.int32, out.shape, 0)
        lane = lax.broadcasted_iota(jnp.int32, out.shape, 1)
        picked = jnp.where((lane >= head * HEAD) & (lane < head * HEAD + HEAD), out, 0.0)
        read_ref[...] = jnp.sum(picked, axis=0, keepdims=True).astype(jnp.bfloat16)


def fill_cache(latent, kv_gain, w_up_key, w_up_value, q_nope, q_rope, rope):
    n_blocks, rows, cols = latent.shape
    out_cols = w_up_key.shape[1]
    heads = out_cols // HEAD
    length = n_blocks * rows
    whole = lambda shape: pl.BlockSpec(shape, lambda b: (0,) * len(shape))
    return pl.pallas_call(
        functools.partial(cache_kernel, n_blocks),
        grid=(n_blocks,),
        out_shape=(
            jax.ShapeDtypeStruct((length, out_cols), jnp.bfloat16),
            jax.ShapeDtypeStruct((length, out_cols), jnp.bfloat16),
            jax.ShapeDtypeStruct((ROPE, length), jnp.bfloat16),
            jax.ShapeDtypeStruct((1, out_cols), jnp.bfloat16),
        ),
        in_specs=[
            pl.BlockSpec((1, rows, cols), lambda b: (b, 0, 0)),
            whole((1, cols)),
            whole((cols, out_cols)),
            whole((cols, out_cols)),
            whole(q_nope.shape),
            whole(q_rope.shape),
            pl.BlockSpec((1, rows, LANES), lambda b: (b, 0, 0)),
        ],
        out_specs=(
            pl.BlockSpec((rows, out_cols), lambda b: (b, 0)),
            pl.BlockSpec((rows, out_cols), lambda b: (b, 0)),
            pl.BlockSpec((ROPE, rows), lambda b: (0, b)),
            whole((1, out_cols)),
        ),
        scratch_shapes=[
            pltpu.VMEM((n_blocks, heads, rows), jnp.float32),
            pltpu.VMEM((n_blocks, rows, out_cols), jnp.bfloat16),
        ],
    )(latent, kv_gain, w_up_key, w_up_value, q_nope, q_rope, rope)


def local(
    tokens, offsets, in_gain, w_latent, w_rope_key, kv_gain, w_up_key, w_up_value, q_nope, q_rope
):
    frequency = np.float32(10000.0) ** (-np.arange(0, ROPE, 2).astype(np.float32) / ROPE)
    inverse = np.zeros((1, LANES), np.float32)
    inverse[0, :ROPE] = np.concatenate([frequency, frequency])
    inverse = jnp.asarray(inverse)
    latent, rope = gather_latent(tokens, w_latent, w_rope_key.T, in_gain[None], offsets, inverse)
    keys, values, rope_keys, read = fill_cache(
        latent, kv_gain[None], w_up_key, w_up_value, q_nope, q_rope, rope
    )
    return (keys[None], values[None], rope_keys[None], read)


def solution(mesh):
    in_specs = (
        P(("grp", "tp"), "sp", None),
        P(("grp", "tp")),
        P(),
        P("sp", None),
        P(),
        P(),
        P(None, "tp"),
        P(None, "tp"),
        P(("grp", "sp"), "tp"),
        P(("grp", "sp"), "tp"),
    )
    out_specs = (
        P(("grp", "sp"), None, "tp"),
        P(("grp", "sp"), None, "tp"),
        P(("grp", "sp"), None, None),
        P(("grp", "sp"), "tp"),
    )
    return jax.shard_map(local, mesh=mesh, in_specs=in_specs, out_specs=out_specs, check_vma=False)
```

```python
import functools

import jax
import jax.numpy as jnp
import numpy as np
from jax import lax
from jax.experimental import pallas as pl
from jax.experimental.pallas import tpu as pltpu
from jax.sharding import PartitionSpec as P

HEAD = 64
ROPE = 32
LANES = 128
CORES = 2
GROUPS = 4
LAGS = (3, 6, 7)
HOP = 3


EPS = 1e-06
MESH = pl.DeviceIdType.MESH


def gather_kernel(
    n_grp,
    n_sp,
    n_tp,
    groups,
    tok_hbm,
    w_hbm,
    w_rope_hbm,
    in_gain,
    offsets,
    inverse,
    lat_out,
    rope_out,
    tok,
    w_own,
    w_rope,
    normed,
    wbuf,
    acc,
    own,
    own_rope,
    transit,
    local_sem,
    own_send,
    z_send,
    z_recv,
    a_send,
    a_recv,
    b_send,
    b_recv,
    c_send,
    c_recv,
    l_send,
    t_send,
    t_recv,
    x_send,
    d_send,
    l_recv,
):
    n_x = n_tp // CORES
    prompts, rows = own.shape[1:3]
    depth, cols = w_own.shape
    width = cols // groups
    chunk = wbuf.shape[5]
    y, z, t = lax.axis_index("grp"), lax.axis_index("sp"), lax.axis_index("tp")
    x, core = t // CORES, t % CORES
    rank = (core * n_x + x) * n_grp + y
    half = n_x // 2

    def tp_of(x_to, core_to):
        return {"tp": x_to * CORES + core_to}

    x_peers = [lax.rem(x + k, n_x) for k in range(1, n_x)]
    y_peers = [lax.rem(y + k, n_grp) for k in range(1, n_grp)]
    z_peers = [lax.rem(z + k, n_sp) for k in range(1, n_sp)]

    fetch_tok = pltpu.make_async_copy(tok_hbm, tok, local_sem.at[0])
    fetch_w = pltpu.make_async_copy(w_hbm, w_own, local_sem.at[1])
    fetch_rope = pltpu.make_async_copy(w_rope_hbm, w_rope, local_sem.at[2])
    fetch_tok.start()
    fetch_w.start()
    fetch_rope.start()

    barrier = pltpu.get_barrier_semaphore()
    targets = (
        [tp_of(p, core) for p in x_peers]
        + [{"grp": p} for p in y_peers]
        + [{"sp": p} for p in z_peers]
        + [tp_of(x, 1 - core)]
    )
    for target in targets:
        pl.semaphore_signal(barrier, inc=1, device_id=target, device_id_type=MESH)
    pl.semaphore_wait(barrier, len(targets))

    finish = []

    def remote(src, dst, send, recv, device):
        return pltpu.make_async_remote_copy(
            src_ref=src,
            dst_ref=dst,
            send_sem=send,
            recv_sem=recv,
            device_id=device,
            device_id_type=MESH,
        )

    def arrived(ref, recv):
        remote(ref, ref, recv, recv, tp_of(x, 1 - core)).wait_recv()

    units = [(g, d) for g in range(groups) for d in range(1, n_sp)]
    above = n_sp - 1 - z
    both = jnp.minimum(z, above)

    def shard(d):
        paired = d <= 2 * both
        hop = jnp.where(paired, (d + 1) // 2, d - both)
        up = jnp.where(paired, d % 2 == 1, above > z)
        return jnp.where(up, z + hop, z - hop), up

    shards = {d: shard(d) for d in range(1, n_sp)}

    def own_z(g):
        for side, ahead, exists in ((0, z + 1, z + 1 < n_sp), (1, z + n_sp - 1, z > 0)):
            copy = remote(
                w_hbm.at[pl.ds(rank * chunk, chunk), pl.ds(g * width, width)],
                wbuf.at[g, z, core, x, y],
                own_send.at[g, side],
                z_recv.at[g, z],
                {"sp": lax.rem(ahead, n_sp)},
            )
            pl.when(exists)(copy.start)
            finish.append(lambda exists=exists, copy=copy: pl.when(exists)(copy.wait_send))

    def pass_z(u):
        g, d = units[u]
        s, up = shards[d]
        exists = jnp.where(up, z > 0, z + 1 < n_sp)
        ahead = jnp.where(up, z + n_sp - 1, z + 1)
        copy = remote(
            block_a(u),
            block_a(u),
            z_send.at[u],
            z_recv.at[g, s],
            {"sp": lax.rem(ahead, n_sp)},
        )
        pl.when(exists)(copy.start)
        finish.append(lambda: pl.when(exists)(copy.wait_send))

    def x_first(u):
        return u % 3 > 0

    def spread(u, src, send, recv, along_x):
        peers = x_peers if along_x else y_peers
        for k, peer in enumerate(peers):
            copy = remote(
                src,
                src,
                send.at[u, k],
                recv.at[u, k],
                tp_of(peer, core) if along_x else {"grp": peer},
            )
            copy.start()
            finish.append(copy.wait_send)

    def block_a(u):
        g, d = units[u]
        return wbuf.at[g, shards[d][0], core, x, y]

    def block_b(u):
        g, d = units[u]
        if x_first(u):
            return wbuf.at[g, shards[d][0], core, :, y]
        return wbuf.at[g, shards[d][0], core, x]

    def stage_a(u):
        arrived(block_a(u), z_recv.at[units[u][0], shards[units[u][1]][0]])
        pass_z(u)
        spread(u, block_a(u), a_send, a_recv, x_first(u))

    def stage_b(u):
        g, _ = units[u]
        for k in range(len(x_peers if x_first(u) else y_peers)):
            arrived(block_a(u), a_recv.at[u, k])
        spread(u, block_b(u), b_send, b_recv, not x_first(u))

    def stage_c(u):
        g, d = units[u]
        for k in range(len(y_peers if x_first(u) else x_peers)):
            arrived(block_b(u), b_recv.at[u, k])
        ref = wbuf.at[g, shards[d][0], core]
        copy = remote(ref, ref, c_send.at[u], c_recv.at[u], tp_of(x, 1 - core))
        copy.start()
        finish.append(copy.wait_send)

    def stage_dot(u):
        g, d = units[u]
        arrived(wbuf.at[g, shards[d][0], core], c_recv.at[u])
        s, _ = shards[d]
        weight = wbuf[g, s].reshape(depth, width)
        acc[g] += jnp.dot(
            normed[s], weight, preferred_element_type=jnp.float32
        )

    def crossing(m):
        return m % 2 == 1 and m < groups and n_x % 2 == 0

    def slot(m, s):
        if m == 0:
            return rope_out.at[s]
        return lat_out.at[m - 1, s]

    def mine(m, i):
        return own_rope.at[i] if m == 0 else own.at[m - 1, i]

    swapped = lax.rem(x + half, n_x) * CORES + core

    def stage_l(m):
        for i in range(prompts):
            home = t * prompts + i
            if crossing(m):
                copy = remote(
                    mine(m, i), transit.at[m, i], l_send.at[m, i], t_recv.at[m, i], {"tp": swapped}
                )
            else:
                copy = remote(
                    mine(m, i), slot(m, z), l_send.at[m, i], l_recv.at[m, z], {"sp": home}
                )
            pl.when(home != z)(copy.start)
            finish.append(lambda home=home, copy=copy: pl.when(home != z)(copy.wait_send))

    def stage_t(m):
        for i in range(prompts):
            home = swapped * prompts + i
            copy = remote(
                transit.at[m, i], slot(m, z), t_send.at[m, i], l_recv.at[m, z], {"sp": home}
            )

            def pass_on(m=m, i=i, copy=copy):
                arrived(transit.at[m, i], t_recv.at[m, i])
                copy.start()

            pl.when(home != z)(pass_on)
            finish.append(lambda home=home, copy=copy: pl.when(home != z)(copy.wait_send))

    owner = z // prompts

    def entry(m, e):
        x_in, core_in = owner // CORES, owner % CORES
        if crossing(m) and e > 0:
            x_in = lax.rem(x_in + half, n_x)
        return x_in, core_in

    def partner_copy(m, e):
        s = lax.rem(z + e, n_sp)
        return remote(slot(m, s), slot(m, s), d_send.at[m, e], l_recv.at[m, s], tp_of(x, 1 - core))

    def stage_x(m, e):
        s = lax.rem(z + e, n_sp)
        x_in, core_in = entry(m, e)
        here = (x == x_in) & (core == core_in)
        copies = [
            remote(slot(m, s), slot(m, s), x_send.at[m, e, k], l_recv.at[m, s], tp_of(peer, core))
            for k, peer in enumerate(x_peers)
        ]

        def enter():
            if e > 0:
                arrived(slot(m, s), l_recv.at[m, s])
            for copy in copies:
                copy.start()
            partner_copy(m, e).start()

        pl.when(here)(enter)

        def drain():
            for copy in copies:
                copy.wait_send()
            partner_copy(m, e).wait_send()

        finish.append(lambda: pl.when(here)(drain))

    def stage_d(m, e):
        s = lax.rem(z + e, n_sp)
        x_in, core_in = entry(m, e)
        here = (x != x_in) & (core == core_in)

        def hand():
            arrived(slot(m, s), l_recv.at[m, s])
            partner_copy(m, e).start()

        pl.when(here)(hand)
        finish.append(lambda: pl.when(here)(partner_copy(m, e).wait_send))

    def stage_end(m, e):
        s = lax.rem(z + e, n_sp)
        _, core_in = entry(m, e)
        pl.when(core != core_in)(lambda: arrived(slot(m, s), l_recv.at[m, s]))

    def finalize(m, value):
        value = value.reshape(prompts, rows, value.shape[-1])
        for i in range(prompts):
            mine(m, i)[...] = value[i]

            def keep(i=i):
                slot(m, z)[...] = value[i]

            pl.when(t * prompts + i == z)(keep)

    for g in range(groups):
        own_z(g)

    step_rows, pieces = 16, 4

    def norm(r, carry):
        at = pl.ds(pl.multiple_of(r * step_rows, step_rows), step_rows)
        wide = tok[at, :].astype(jnp.float32)
        scale = lax.rsqrt(jnp.mean(wide * wide, axis=-1, keepdims=True) + EPS)
        out = (wide * scale * in_gain[...]).astype(jnp.bfloat16)
        for b in range(n_sp):
            normed[b, at, :] = out[:, b * depth : (b + 1) * depth]
        return carry

    def norm_piece(k):
        turns = prompts * rows // step_rows // pieces
        lax.fori_loop(k * turns, (k + 1) * turns, norm, 0)

    work = {}

    def at_step(step, fn, *args):
        work.setdefault(step, []).append((fn, args))

    def own_dot(g):
        acc[g] = jnp.dot(
            normed[z], w_own[:, g * width : (g + 1) * width], preferred_element_type=jnp.float32
        )

    def rope_item():
        fetch_rope.wait()
        raw = jnp.zeros((prompts * rows, ROPE), jnp.float32)
        for b in range(n_sp):
            raw += lax.dot_general(
                normed[b],
                w_rope[:, b * depth : (b + 1) * depth],
                (((1,), (1,)), ((), ())),
                preferred_element_type=jnp.float32,
            )
        half_rope = ROPE // 2
        blank = jnp.zeros((prompts * rows, LANES - ROPE), jnp.float32)
        lane = lax.broadcasted_iota(jnp.int32, (rows, LANES), 1)
        index = lax.broadcasted_iota(jnp.int32, (rows, LANES), 0)
        plain = jnp.concatenate([raw, blank], axis=1)
        other = jnp.concatenate([raw[:, half_rope:], raw[:, :half_rope], blank], axis=1)
        turned = []
        for i in range(prompts):
            position = offsets[i] + z * rows + index
            angle = position.astype(jnp.float32) * inverse[...]
            sine = jnp.sin(angle)
            sine = jnp.where(lane < half_rope, -sine, sine)
            at = slice(i * rows, (i + 1) * rows)
            turned.append(plain[at] * jnp.cos(angle) + other[at] * sine)
        finalize(0, jnp.concatenate(turned, axis=0).astype(jnp.bfloat16))

    def group_item(g):
        finalize(g + 1, acc[g].astype(jnp.bfloat16))

    def route(m, step):
        at_step(step, stage_l, m)
        if crossing(m):
            step += HOP
            at_step(step, stage_t, m)
        for e in range(n_sp):
            at_step(step + HOP, stage_x, m, e)
        for e in range(n_sp):
            at_step(step + 2 * HOP, stage_d, m, e)

    lag_b, lag_c, lag_dot = LAGS
    for u, (g, d) in enumerate(units):
        at_step(u, stage_a, u)
        at_step(u + lag_b, stage_b, u)
        at_step(u + lag_c, stage_c, u)
    at_step(0, fetch_tok.wait)
    for k in range(pieces):
        at_step(k, norm_piece, k)
    at_step(pieces, fetch_w.wait)
    at_step(pieces, rope_item)
    route(0, pieces)
    for u, (g, d) in enumerate(units):
        step = max(u + lag_dot, pieces)
        if d == 1:
            at_step(step, own_dot, g)
        at_step(step, stage_dot, u)
        if d == n_sp - 1:
            at_step(step, group_item, g)
            route(g + 1, step)

    for step in sorted(work):
        for fn, args in work[step]:
            fn(*args)
    for m in range(groups + 1):
        for e in range(n_sp):
            stage_end(m, e)
    for fn in finish:
        fn()


def gather_latent(tokens, w_latent, w_rope, in_gain, offsets, inverse):
    prompts, rows, width = tokens.shape
    n_grp, n_sp, n_tp = (lax.axis_size(a) for a in ("grp", "sp", "tp"))
    n_x = n_tp // CORES
    depth, cols = w_latent.shape
    groups = max(1, GROUPS * 3 // (n_sp - 1) // 4 * 4)
    part = cols // groups
    chunk = depth // (n_grp * n_tp)
    total = prompts * rows
    units = groups * (n_sp - 1)
    peers = max(n_x, n_grp) - 1
    items = groups + 1
    bf16, f32 = jnp.bfloat16, jnp.float32
    dma = pltpu.SemaphoreType.DMA
    vmem = pl.BlockSpec(memory_space=pltpu.VMEM)
    hbm = pl.BlockSpec(memory_space=pl.ANY)
    return pl.pallas_call(
        functools.partial(gather_kernel, n_grp, n_sp, n_tp, groups),
        out_shape=(
            jax.ShapeDtypeStruct((groups, n_sp, rows, part), bf16),
            jax.ShapeDtypeStruct((n_sp, rows, LANES), bf16),
        ),
        in_specs=[hbm, hbm, hbm, vmem, pl.BlockSpec(memory_space=pltpu.SMEM), vmem],
        out_specs=(vmem, vmem),
        scratch_shapes=[
            pltpu.VMEM((total, width), bf16),
            pltpu.VMEM((depth, cols), bf16),
            pltpu.VMEM((ROPE, width), bf16),
            pltpu.VMEM((n_sp, total, depth), bf16),
            pltpu.VMEM((groups, n_sp, CORES, n_x, n_grp, chunk, part), bf16),
            pltpu.VMEM((groups, total, part), f32),
            pltpu.VMEM((groups, prompts, rows, part), bf16),
            pltpu.VMEM((prompts, rows, LANES), bf16),
            pltpu.VMEM((items, prompts, rows, part), bf16),
            dma((3,)),
            dma((groups, 2)),
            dma((units,)),
            dma((groups, n_sp)),
            dma((units, peers)),
            dma((units, peers)),
            dma((units, peers)),
            dma((units, peers)),
            dma((units,)),
            dma((units,)),
            dma((items, prompts)),
            dma((items, prompts)),
            dma((items, prompts)),
            dma((items, n_sp, max(n_x - 1, 1))),
            dma((items, n_sp)),
            dma((items, n_sp)),
        ],
        compiler_params=pltpu.CompilerParams(
            collective_id=0, has_side_effects=True, vmem_limit_bytes=60 * 1024 * 1024
        ),
    )(tokens.reshape(total, width), w_latent, w_rope, in_gain, offsets, inverse)


def cache_kernel(
    n_blocks,
    latent_ref,
    gain_ref,
    wk_ref,
    wv_ref,
    q_nope_ref,
    q_rope_ref,
    rope_ref,
    keys_ref,
    values_ref,
    rope_keys_ref,
    read_ref,
    scores,
    held,
):
    b = pl.program_id(0)
    heads = scores.shape[1]

    def per_head(row, size):
        wide = jnp.broadcast_to(row.astype(jnp.float32), (heads, heads * size))
        head = lax.broadcasted_iota(jnp.int32, wide.shape, 0)
        lane = lax.broadcasted_iota(jnp.int32, wide.shape, 1)
        return jnp.where((lane >= head * size) & (lane < head * size + size), wide, 0.0)

    query = per_head(q_nope_ref[...], HEAD).astype(jnp.bfloat16)
    spread = (heads * ROPE, LANES)
    fold = lax.broadcasted_iota(jnp.int32, spread, 0) % ROPE == lax.broadcasted_iota(
        jnp.int32, spread, 1
    )
    rotary_q = jnp.dot(
        per_head(q_rope_ref[...], ROPE).astype(jnp.bfloat16),
        jnp.where(fold, 1.0, 0.0).astype(jnp.bfloat16),
        preferred_element_type=jnp.float32,
    ).astype(jnp.bfloat16)
    parts = [latent_ref[g, 0] for g in range(latent_ref.shape[0])]
    raw = jnp.concatenate(parts, axis=1).astype(jnp.float32)
    scale = lax.rsqrt(jnp.mean(raw * raw, axis=-1, keepdims=True) + EPS)
    latent = (raw * scale * gain_ref[...]).astype(jnp.bfloat16)
    keys = jnp.dot(latent, wk_ref[...], preferred_element_type=jnp.float32).astype(jnp.bfloat16)
    keys_ref[...] = keys
    values = jnp.dot(latent, wv_ref[...], preferred_element_type=jnp.float32).astype(jnp.bfloat16)
    values_ref[...] = values
    held[b] = values
    rope = rope_ref[0]
    rope_keys_ref[...] = rope.astype(jnp.float32).T[:ROPE].astype(jnp.bfloat16)
    across = (((1,), (1,)), ((), ()))
    part = lax.dot_general(query, keys, across, preferred_element_type=jnp.float32)
    part += lax.dot_general(rotary_q, rope, across, preferred_element_type=jnp.float32)
    scores[b] = part / jnp.sqrt(jnp.float32(HEAD + ROPE))

    @pl.when(b == n_blocks - 1)
    def _():
        every = scores[...]
        peak = jnp.max(jnp.max(every, axis=-1, keepdims=True), axis=0, keepdims=True)
        expo = jnp.exp(every - peak)
        total = jnp.sum(jnp.sum(expo, axis=-1, keepdims=True), axis=0, keepdims=True)
        weights = (expo / total).astype(jnp.bfloat16)
        out = jnp.dot(weights[0], held[0], preferred_element_type=jnp.float32)
        for i in range(1, n_blocks):
            out += jnp.dot(weights[i], held[i], preferred_element_type=jnp.float32)
        head = lax.broadcasted_iota(jnp.int32, out.shape, 0)
        lane = lax.broadcasted_iota(jnp.int32, out.shape, 1)
        picked = jnp.where((lane >= head * HEAD) & (lane < head * HEAD + HEAD), out, 0.0)
        read_ref[...] = jnp.sum(picked, axis=0, keepdims=True).astype(jnp.bfloat16)


def fill_cache(latent, kv_gain, w_up_key, w_up_value, q_nope, q_rope, rope):
    groups, n_blocks, rows, part = latent.shape
    cols = groups * part
    out_cols = w_up_key.shape[1]
    heads = out_cols // HEAD
    length = n_blocks * rows
    whole = lambda shape: pl.BlockSpec(shape, lambda b: (0,) * len(shape))
    return pl.pallas_call(
        functools.partial(cache_kernel, n_blocks),
        grid=(n_blocks,),
        out_shape=(
            jax.ShapeDtypeStruct((length, out_cols), jnp.bfloat16),
            jax.ShapeDtypeStruct((length, out_cols), jnp.bfloat16),
            jax.ShapeDtypeStruct((ROPE, length), jnp.bfloat16),
            jax.ShapeDtypeStruct((1, out_cols), jnp.bfloat16),
        ),
        in_specs=[
            pl.BlockSpec((groups, 1, rows, part), lambda b: (0, b, 0, 0)),
            whole((1, cols)),
            whole((cols, out_cols)),
            whole((cols, out_cols)),
            whole(q_nope.shape),
            whole(q_rope.shape),
            pl.BlockSpec((1, rows, LANES), lambda b: (b, 0, 0)),
        ],
        out_specs=(
            pl.BlockSpec((rows, out_cols), lambda b: (b, 0)),
            pl.BlockSpec((rows, out_cols), lambda b: (b, 0)),
            pl.BlockSpec((ROPE, rows), lambda b: (0, b)),
            whole((1, out_cols)),
        ),
        scratch_shapes=[
            pltpu.VMEM((n_blocks, heads, rows), jnp.float32),
            pltpu.VMEM((n_blocks, rows, out_cols), jnp.bfloat16),
        ],
    )(latent, kv_gain, w_up_key, w_up_value, q_nope, q_rope, rope)


def local(
    tokens, offsets, in_gain, w_latent, w_rope_key, kv_gain, w_up_key, w_up_value, q_nope, q_rope
):
    frequency = np.float32(10000.0) ** (-np.arange(0, ROPE, 2).astype(np.float32) / ROPE)
    inverse = np.zeros((1, LANES), np.float32)
    inverse[0, :ROPE] = np.concatenate([frequency, frequency])
    inverse = jnp.asarray(inverse)
    latent, rope = gather_latent(tokens, w_latent, w_rope_key.T, in_gain[None], offsets, inverse)
    keys, values, rope_keys, read = fill_cache(
        latent, kv_gain[None], w_up_key, w_up_value, q_nope, q_rope, rope
    )
    return (keys[None], values[None], rope_keys[None], read)


def solution(mesh):
    in_specs = (
        P(("grp", "tp"), "sp", None),
        P(("grp", "tp")),
        P(),
        P("sp", None),
        P(),
        P(),
        P(None, "tp"),
        P(None, "tp"),
        P(("grp", "sp"), "tp"),
        P(("grp", "sp"), "tp"),
    )
    out_specs = (
        P(("grp", "sp"), None, "tp"),
        P(("grp", "sp"), None, "tp"),
        P(("grp", "sp"), None, None),
        P(("grp", "sp"), "tp"),
    )
    return jax.shard_map(local, mesh=mesh, in_specs=in_specs, out_specs=out_specs, check_vma=False)
```
